32 devices in a mesh: fs: 8 (over z, y), tp: 4 (over x, core).
Axes of the slice: x: 2, y: 2, z: 4, core: 2. Of those that a mesh axis runs over, the one named last changes fastest.
Arguments:
- tokens: bfloat16 [4096, 2048], P(('fs', 'tp')), may hold values from -6 to 6
- routes: int32 [4096, 4], P(('fs', 'tp')), may hold values from 0 to 31, all different within a row; in each aligned block of 128 rows (0 to 127, 128 to 255, ...) at most 24 rows name the same one
- route_weight: float32 [4096, 4], P(('fs', 'tp')), may hold values from 0.1 to 1
- norm_gain: float32 [2048], P('fs'), may hold values from 0.5 to 4
- gate_weight: float32 [32, 2048, 512], P(None, 'fs', 'tp'), may hold values from -0.125 to 0.125
- up_weight: float32 [32, 2048, 512], P(None, 'fs', 'tp'), may hold values from -0.125 to 0.125
- down_weight: float32 [32, 512, 2048], P(None, 'fs', 'tp'), may hold values from -0.0625 to 0.0625
Outputs:
- gate_new: bfloat16 [32, 2048, 512], P(('fs', 'tp'))
- up_new: bfloat16 [32, 2048, 512], P(('fs', 'tp'))
- down_new: bfloat16 [32, 512, 2048], P(('fs', 'tp'))
- mixed: bfloat16 [4096, 2048], P(('fs', 'tp'))
The draws below stay inside these ranges and needn't reach their ends.
Inputs may be any that keep to these rules, and one draw needn't show every extreme that they name: `routes`: each row names 4 different experts, and every expert is named by some row; within the 128 rows of one device no expert is named by more than 24 rows, and in some blocks an expert is named by exactly 24 rows.
All inputs are finite; a program needn't handle non-finite values.
Results may differ from the reference program's by a relative error of at most 0.0084.
Values may be sent and summed in bfloat16 or wider, within the bound.
A program may use at most 128 MiB of HBM per device.

```python
import math
import jax
import jax.numpy as jnp
import numpy as np
from jax import lax

D = 2048
FF = 512
TOP_K = 4
TOK_DEV = 128
EXPERTS = 32
CAP = 24
TOKENS = 4096
N_FS = 8
N_TP = 4


def shard_levels(rng, shape, shards, least, largest):
    loudness, own = 1.0, jax.random.fold_in(rng, 6)
    for position, parts in shards:
        draws = jnp.exp(jax.random.uniform(jax.random.fold_in(own, position), (parts,), jnp.float32, least / len(shards), largest / len(shards)))
        loudness = loudness * jnp.repeat(draws, shape[position] // parts).reshape([-1 if axis == position else 1 for axis in range(len(shape))])
    return loudness


def shared_out(rng, own, number, rows, amount, top, reach, skew):
    ranking = jax.random.permutation(rng, amount)
    heavy_load, usual = portions_of(amount, rows * top, reach, skew, True), portions_of(amount, rows * top, reach, skew, False)
    places = jnp.arange(amount)

    def named(lengths, turn):
        used = int((lengths > 0).sum())
        fixed = max(1, used // 4)
        shifted = fixed + (places - fixed + turn * (used - fixed)) % max(1, amount - fixed)
        return jnp.zeros((amount,), jnp.int32).at[ranking[jnp.where(places < fixed, places, shifted)]].set(jnp.asarray(lengths, jnp.int32))

    lengths = jnp.where(number % 4 == 0, named(heavy_load, number // 4), named(usual, number - number // 4 - 1))
    mixed = jax.random.permutation(jax.random.fold_in(own, 3), amount)
    giver, sink = mixed[0:amount // 2 * 2:2], mixed[1:amount // 2 * 2:2]
    slack = jnp.minimum(lengths[giver] - 1, reach - lengths[sink]) // 2
    slack = jnp.where((giver == ranking[0]) | (sink == ranking[0]) | (lengths[sink] == 0), 0, jnp.maximum(slack, 0))
    shifted = jax.random.randint(jax.random.fold_in(own, 4), (amount // 2,), 0, 1 << 20) % (slack + 1)
    lengths = lengths.at[giver].add(-shifted).at[sink].add(shifted)
    members = jnp.searchsorted(jnp.cumsum(lengths), jnp.arange(rows * top), side="right").astype(jnp.int32)
    listing = members.reshape(top, rows).T
    listing = listing[jax.random.permutation(jax.random.fold_in(own, 1), rows)]
    turn = jax.random.randint(jax.random.fold_in(own, 2), (rows, 1), 0, top)
    return jnp.take_along_axis(listing, (jnp.arange(top)[None, :] + turn) % top, axis=1)


def portions_of(number_of, total, most, lean, full):
    weights = [(1 << 20) // math.isqrt(rank ** lean) + 1 for rank in range(1, number_of + 1)]
    largest = most if full else min(most, max(-(-total // number_of), total * weights[0] // sum(weights)))
    least = 1 if total - largest >= number_of - 1 else 0
    given, rest = [largest] + [least] * (number_of - 1), total - largest - least * (number_of - 1)
    while rest > 0:
        free = [i for i in range(1, number_of) if given[i] < largest] or [i for i in range(1, number_of) if given[i] < most]
        whole, remaining = sum([weights[i] for i in free]), rest
        for i in free:
            extra = min(most - given[i], max(1, remaining * weights[i] // whole), rest)
            given[i] = given[i] + extra
            rest = rest - extra
    return np.array(given)


def noise(stream_key, shape, deviation, most, split=(), held_as=jnp.bfloat16):
    values = jax.random.normal(stream_key, shape, jnp.float32) * deviation
    if len(split) > 0:
        values = shard_levels(stream_key, shape, split, -0.22, 0.18) * values
    return jnp.clip(values, min=-most, max=most).astype(held_as)


def setup_inputs(seed: int = 0) -> dict:
    streams_of = jax.random.split(jax.random.key(seed), 8)
    tokens = noise(streams_of[0], (TOKENS, D), 1.0, 6.0, ((0, 32),))
    routes_keys = jax.random.split(jax.random.fold_in(streams_of[1], 1), TOKENS // TOK_DEV)
    routes_turns = jax.random.permutation(jax.random.fold_in(streams_of[1], 3), TOKENS // TOK_DEV)
    routes = jax.vmap(lambda own, number: shared_out(jax.random.fold_in(streams_of[1], 2), own, number, TOK_DEV, EXPERTS, TOP_K, CAP, 1))(routes_keys, routes_turns).reshape((TOKENS, TOP_K))
    route_weight = jnp.clip(jnp.exp(math.log(1.0) - 2.3025851 * jax.random.uniform(streams_of[2], (TOKENS, TOP_K), jnp.float32) ** shard_levels(streams_of[2], (TOKENS, TOP_K), ((0, 32),), -0.2, 0.2)), 0.1, 1.0)
    norm_gain = jnp.clip(jnp.exp(math.log(4.0) - 2.0794415 * jax.random.uniform(streams_of[3], (D,), jnp.float32) ** shard_levels(streams_of[3], (D,), ((0, 8),), -0.2, 0.2)), 0.5, 4.0)
    gate_weight = noise(streams_of[4], (EXPERTS, D, FF), D ** -0.5, 0.125, ((1, 8), (2, 4)), jnp.float32)
    up_weight = noise(streams_of[5], (EXPERTS, D, FF), D ** -0.5, 0.125, ((1, 8), (2, 4)), jnp.float32)
    down_weight = noise(streams_of[6], (EXPERTS, FF, D), (16 * FF) ** -0.5, 0.0625, ((1, 8), (2, 4)), jnp.float32)
    return {"tokens": tokens, "routes": routes, "route_weight": route_weight, "norm_gain": norm_gain, "gate_weight": gate_weight, "up_weight": up_weight, "down_weight": down_weight}


norm_epsilon = 1e-06
clamp_limit = 7.0
sigmoid_slope = 1.702

def feed(inputs, gate_mat, up_mat, down_mat):
    gate_pre = jnp.dot(inputs, gate_mat, preferred_element_type=jnp.float32)
    up_pre = jnp.dot(inputs, up_mat, preferred_element_type=jnp.float32)
    gate_part = jnp.minimum(gate_pre, clamp_limit)
    linear_part = jnp.clip(up_pre, -clamp_limit, clamp_limit)
    activation = (gate_part * jax.nn.sigmoid(sigmoid_slope * gate_part) * (linear_part + 1.0)).astype(jnp.bfloat16)
    return jnp.dot(activation, down_mat, preferred_element_type=jnp.float32).astype(jnp.bfloat16)

def reference(tokens, routes, route_weight, norm_gain, gate_weight, up_weight, down_weight):
    gate_all = (gate_weight * norm_gain[None, :, None]).astype(jnp.bfloat16)
    up_all = (up_weight * norm_gain[None, :, None]).astype(jnp.bfloat16)
    down_all = down_weight.astype(jnp.bfloat16)
    values = tokens.astype(jnp.float32)
    squares = lax.optimization_barrier(jnp.mean(values * values, axis=1, keepdims=True))
    normed = (values * lax.rsqrt(squares + norm_epsilon)).astype(jnp.bfloat16)
    devices = N_FS * N_TP
    pair_experts = routes.reshape(devices, TOK_DEV * TOP_K)
    onehot = (pair_experts[:, :, None] == jnp.arange(EXPERTS, dtype=jnp.int32)[None, None, :]).astype(jnp.int32)
    earlier = jnp.cumsum(onehot, axis=1) - onehot
    rank = lax.optimization_barrier(jnp.sum(earlier * onehot, axis=2)).astype(jnp.int32)
    source_dev = jnp.arange(devices, dtype=jnp.int32)[:, None]
    column = (source_dev * CAP + rank).astype(jnp.int32)
    token_index = (source_dev * TOK_DEV + jnp.arange(TOK_DEV * TOP_K, dtype=jnp.int32)[None, :] // TOP_K).astype(jnp.int32)
    slot_table = jnp.full((EXPERTS, devices * CAP), TOKENS, jnp.int32).at[pair_experts, column].set(token_index)
    padded = jnp.concatenate([normed, jnp.zeros((1, D), jnp.bfloat16)], axis=0)

    def expert_rows(operands):
        rows_index, gate_mat, up_mat, down_mat = operands
        return feed(padded[rows_index], gate_mat, up_mat, down_mat)
    returned = lax.map(expert_rows, (slot_table, gate_all, up_all, down_all))
    picked = returned[pair_experts, column].reshape(TOKENS, TOP_K, D)
    mixed = lax.optimization_barrier(jnp.sum(picked.astype(jnp.float32) * route_weight[:, :, None], axis=1)).astype(jnp.bfloat16)
    return (gate_all, up_all, down_all, mixed)
```

```python
import functools

import jax
import jax.numpy as jnp
from jax import lax
from jax.experimental import pallas as pl
from jax.experimental.pallas import tpu as pltpu
from jax.sharding import PartitionSpec as P

norm_epsilon = 1e-06
clamp_limit = 7.0
sigmoid_slope = 1.702
MESH = pl.DeviceIdType.MESH


def feed(inputs, gate_mat, up_mat, down_mat):
    gate_pre = jnp.dot(inputs, gate_mat, preferred_element_type=jnp.float32)
    up_pre = jnp.dot(inputs, up_mat, preferred_element_type=jnp.float32)
    gate_part = jnp.minimum(gate_pre, clamp_limit)
    linear_part = jnp.clip(up_pre, -clamp_limit, clamp_limit)
    activation = (
        gate_part * jax.nn.sigmoid(sigmoid_slope * gate_part) * (linear_part + 1.0)
    ).astype(jnp.bfloat16)
    return jnp.dot(activation, down_mat, preferred_element_type=jnp.float32).astype(jnp.bfloat16)


def assemble(received, rows_groups, column_groups):
    tile_rows = received.shape[2]
    tile_columns = received.shape[3]
    sources = received.reshape(rows_groups, column_groups, tile_rows, tile_columns)
    return sources.transpose(0, 2, 1, 3).reshape(
        1, rows_groups * tile_rows, column_groups * tile_columns
    )


def shards(tokens, routes, route_weight, norm_gain, gate_weight, up_weight, down_weight):
    gain_column = norm_gain[None, :, None]
    gate_tiles = (gate_weight * gain_column).astype(jnp.bfloat16)
    up_tiles = (up_weight * gain_column).astype(jnp.bfloat16)
    down_tiles = down_weight.astype(jnp.bfloat16)
    rows_groups = lax.axis_size("fs")
    column_groups = lax.axis_size("tp")
    arrived = (
        lax.all_to_all(gate_tiles[:, None], ("fs", "tp"), split_axis=0, concat_axis=1, tiled=True),
        lax.all_to_all(up_tiles[:, None], ("fs", "tp"), split_axis=0, concat_axis=1, tiled=True),
        lax.all_to_all(down_tiles[:, None], ("fs", "tp"), split_axis=0, concat_axis=1, tiled=True),
    )
    gate_new = assemble(arrived[0], rows_groups, column_groups)
    up_new = assemble(arrived[1], rows_groups, column_groups)
    down_new = assemble(arrived[2], rows_groups, column_groups)
    experts = rows_groups * column_groups
    tok_rows, model_width = tokens.shape
    per_token = routes.shape[1]
    capacity = max(2, 3 * tok_rows * per_token // (2 * experts))
    values = tokens.astype(jnp.float32)
    squares = jnp.mean(values * values, axis=1, keepdims=True)
    normed = (values * lax.rsqrt(squares + norm_epsilon)).astype(jnp.bfloat16)
    flat_routes = routes.reshape(-1)
    onehot = (flat_routes[:, None] == jnp.arange(experts, dtype=jnp.int32)[None, :]).astype(
        jnp.int32
    )
    earlier = jnp.cumsum(onehot, axis=0) - onehot
    rank = jnp.sum(earlier * onehot, axis=1)
    slot_index = flat_routes * capacity + rank
    slot_numbers = jnp.arange(experts * capacity, dtype=jnp.int32)
    select = jnp.any(
        slot_index.reshape(tok_rows, per_token)[None, :, :] == slot_numbers[:, None, None], axis=2
    )
    buffer = jnp.dot(
        select.astype(jnp.bfloat16), normed, preferred_element_type=jnp.float32
    ).astype(jnp.bfloat16)
    buffer = buffer.reshape(experts, 1, capacity, model_width)
    slot_rows = lax.all_to_all(buffer, ("fs", "tp"), split_axis=0, concat_axis=1, tiled=True)
    sources = slot_rows.shape[1]
    count = slot_rows.shape[2]
    expert_out = feed(slot_rows.reshape(-1, model_width), gate_new[0], up_new[0], down_new[0])
    expert_out = expert_out.reshape(1, sources, count, model_width)
    returned = lax.all_to_all(expert_out, ("fs", "tp"), split_axis=1, concat_axis=0, tiled=True)
    returned = returned.reshape(experts * capacity, model_width)
    picked = returned[slot_index].reshape(tok_rows, per_token, model_width)
    mixed = jnp.sum(picked.astype(jnp.float32) * route_weight[:, :, None], axis=1).astype(
        jnp.bfloat16
    )
    return (gate_new, up_new, down_new, mixed)


def exchange_kernel(
    sizes, tokens, routes_t, weight_t, gain, gate, up, down,
    gate_out, up_out, down_out, mixed,
    gate_in, up_in, down_in, in_tiles, out_tiles, in_mats, out_mat,
    slots_out, slots_in, active, ranks, picks, mix_high, mix_low, rows_out, rows_in,
    load_sem, store_sem, slot_send, slot_recv, first_send, first_recv,
    second_send, second_recv, back_send, back_recv,
):
    n_fs, n_tp, capacity = sizes
    n = n_fs * n_tp
    fs, tp = lax.axis_index("fs"), lax.axis_index("tp")
    me = fs * n_tp + tp
    tok_rows, width = tokens.shape
    tile_rows, tile_cols = gate_in.shape[1:]
    down_rows, down_cols = down_in.shape[1:]
    group = 8
    groups = n // group
    group_rows = group * capacity

    def peer(step):
        to_fs = lax.rem(fs + step // n_tp, n_fs)
        to_tp = lax.rem(tp + lax.rem(step, n_tp), n_tp)
        return to_fs, to_tp, to_fs * n_tp + to_tp

    barrier = pltpu.get_barrier_semaphore()

    def greet(step, carry):
        to_fs, to_tp, _ = peer(step)
        pl.semaphore_signal(barrier, inc=1, device_id=(to_fs, to_tp), device_id_type=MESH)
        return carry

    loads = [
        pltpu.make_async_copy(gate, gate_in, load_sem.at[0]),
        pltpu.make_async_copy(up, up_in, load_sem.at[1]),
        pltpu.make_async_copy(down, down_in, load_sem.at[2]),
    ]
    for load in loads:
        load.start()
    lax.fori_loop(1, n, greet, 0)

    experts = lax.broadcasted_iota(jnp.int32, (n, tok_rows), 0)
    named = jnp.zeros((n, tok_rows), jnp.float32)
    scaled = jnp.zeros((n, tok_rows), jnp.float32)
    for k in range(routes_t.shape[0]):
        hit = routes_t[k : k + 1, :] == experts
        named = named + hit.astype(jnp.float32)
        scaled = scaled + jnp.where(hit, weight_t[k : k + 1, :], 0.0)
    before = (
        lax.broadcasted_iota(jnp.int32, (tok_rows, tok_rows), 0)
        < lax.broadcasted_iota(jnp.int32, (tok_rows, tok_rows), 1)
    ).astype(jnp.float32).astype(jnp.bfloat16)
    rank = jnp.dot(named.astype(jnp.bfloat16), before, preferred_element_type=jnp.float32)
    ranks[...] = jnp.where(named > 0.5, rank, -1.0)
    values = tokens[...].astype(jnp.float32)
    squares = jnp.mean(values * values, axis=1, keepdims=True)
    normed = (values * lax.rsqrt(squares + norm_epsilon)).astype(jnp.bfloat16)
    for g in range(groups):
        held = slice(g * group, (g + 1) * group)
        number = lax.broadcasted_iota(jnp.int32, (group, capacity, tok_rows), 1).astype(jnp.float32)
        select = (ranks[held, :][:, None, :] == number).astype(jnp.float32)
        picks[g * group_rows : (g + 1) * group_rows, :] = (
            select * scaled[held, :][:, None, :]
        ).reshape(group_rows, tok_rows)
        rows = jnp.dot(
            select.reshape(group_rows, tok_rows).astype(jnp.bfloat16),
            normed,
            preferred_element_type=jnp.float32,
        )
        slots_out[held] = rows.reshape(group, capacity, width).astype(jnp.bfloat16)

    pl.semaphore_wait(barrier, n - 1)

    def slot_copy(to, source):
        return pltpu.make_async_remote_copy(
            src_ref=slots_out.at[to[2]],
            dst_ref=slots_in.at[source],
            send_sem=slot_send.at[to[2]],
            recv_sem=slot_recv.at[source],
            device_id=(to[0], to[1]),
            device_id_type=MESH,
        )

    def first_copy(to, place):
        return pltpu.make_async_remote_copy(
            src_ref=in_tiles.at[to[2]],
            dst_ref=in_mats.at[
                :,
                pl.ds(pl.multiple_of(place[0] * tile_rows, tile_rows), tile_rows),
                pl.ds(pl.multiple_of(place[1] * tile_cols, tile_cols), tile_cols),
            ],
            send_sem=first_send.at[to[2]],
            recv_sem=first_recv.at[place[2]],
            device_id=(to[0], to[1]),
            device_id_type=MESH,
        )

    def second_copy(to, place):
        return pltpu.make_async_remote_copy(
            src_ref=out_tiles.at[to[2]],
            dst_ref=out_mat.at[
                pl.ds(pl.multiple_of(place[0] * down_rows, down_rows), down_rows),
                pl.ds(pl.multiple_of(place[1] * down_cols, down_cols), down_cols),
            ],
            send_sem=second_send.at[to[2]],
            recv_sem=second_recv.at[place[2]],
            device_id=(to[0], to[1]),
            device_id_type=MESH,
        )

    def back_copy(to, source):
        return pltpu.make_async_remote_copy(
            src_ref=rows_out.at[to[2]],
            dst_ref=rows_in.at[source],
            send_sem=back_send.at[to[2]],
            recv_sem=back_recv.at[source],
            device_id=(to[0], to[1]),
            device_id_type=MESH,
        )

    mine = (fs, tp, me)

    def send_slots(step, carry):
        slot_copy(peer(step), me).start()
        return carry

    lax.fori_loop(1, n, send_slots, 0)
    slots_in[me] = slots_out[me]

    loads[0].wait()
    loads[1].wait()
    gains = jnp.broadcast_to(gain[...], (tile_rows, tile_cols))

    def cast_first(step):
        e = peer(step)[2]
        in_tiles[e, 0] = (gate_in[e] * gains).astype(jnp.bfloat16)
        in_tiles[e, 1] = (up_in[e] * gains).astype(jnp.bfloat16)

    cast_first(1)

    def send_first(step, carry):
        cast_first(step + 1)
        first_copy(peer(step), mine).start()
        return carry

    lax.fori_loop(1, n, send_first, 0)
    own_rows = pl.ds(pl.multiple_of(fs * tile_rows, tile_rows), tile_rows)
    own_cols = pl.ds(pl.multiple_of(tp * tile_cols, tile_cols), tile_cols)
    in_mats[0, own_rows, own_cols] = in_tiles[me, 0]
    in_mats[1, own_rows, own_cols] = in_tiles[me, 1]

    loads[2].wait()

    def cast_second(step):
        e = peer(step)[2]
        out_tiles[e] = down_in[e].astype(jnp.bfloat16)

    cast_second(1)

    def send_second(step, carry):
        cast_second(step + 1)
        second_copy(peer(step), mine).start()
        return carry

    lax.fori_loop(1, n, send_second, 0)
    out_mat[
        pl.ds(pl.multiple_of(fs * down_rows, down_rows), down_rows),
        pl.ds(pl.multiple_of(tp * down_cols, down_cols), down_cols),
    ] = out_tiles[me]

    shares = jnp.transpose(picks[...])
    high = shares.astype(jnp.bfloat16)
    mix_high[...] = high
    mix_low[...] = (shares - high.astype(jnp.float32)).astype(jnp.bfloat16)

    def take_first(step, carry):
        from_ = peer(step)
        slot_copy(mine, from_[2]).wait_recv()
        first_copy(mine, from_).wait_recv()
        return carry

    lax.fori_loop(1, n, take_first, 0)
    stores = [
        pltpu.make_async_copy(in_mats.at[0], gate_out.at[0], store_sem.at[0]),
        pltpu.make_async_copy(in_mats.at[1], up_out.at[0], store_sem.at[1]),
        pltpu.make_async_copy(out_mat, down_out.at[0], store_sem.at[2]),
    ]
    stores[0].start()
    stores[1].start()

    def activate(g, carry):
        inputs = slots_in[pl.ds(g * group, group)].astype(jnp.float32)
        inputs = inputs.reshape(group_rows, width).astype(jnp.bfloat16)
        gate_pre = jnp.dot(inputs, in_mats[0], preferred_element_type=jnp.float32)
        up_pre = jnp.dot(inputs, in_mats[1], preferred_element_type=jnp.float32)
        gate_part = jnp.minimum(gate_pre, clamp_limit)
        linear_part = jnp.clip(up_pre, -clamp_limit, clamp_limit)
        active[g] = (
            gate_part * jax.nn.sigmoid(sigmoid_slope * gate_part) * (linear_part + 1.0)
        ).astype(jnp.bfloat16)
        return carry

    lax.fori_loop(0, groups, activate, 0)

    def take_second(step, carry):
        second_copy(mine, peer(step)).wait_recv()
        return carry

    lax.fori_loop(1, n, take_second, 0)
    stores[2].start()
    home = me // group

    def project(c):
        g = lax.rem(home + c, groups)
        rows = jnp.dot(active[g], out_mat[...], preferred_element_type=jnp.float32)
        rows_out[pl.ds(g * group, group)] = rows.reshape(group, capacity, width).astype(
            jnp.bfloat16
        )

    def send_group(c):
        g = lax.rem(home + c, groups)

        def send_back(step, carry):
            to = g * group + lax.rem(me + step, group)

            @pl.when(to != me)
            def _():
                back_copy((to // n_tp, lax.rem(to, n_tp), to), me).start()

            return carry

        lax.fori_loop(0, group, send_back, 0)

    project(0)

    def return_group(c, carry):
        project(c)
        send_group(c - 1)
        return carry

    lax.fori_loop(1, groups, return_group, 0)
    send_group(groups - 1)
    rows_in[me] = rows_out[me]

    def take_back(step, carry):
        back_copy(mine, peer(step)[2]).wait_recv()
        return carry

    lax.fori_loop(1, n, take_back, 0)
    block = 512

    def mix(c, carry):
        cols = pl.ds(pl.multiple_of(c * block, block), block)
        rows = rows_in[:, :, cols].astype(jnp.float32).reshape(n * capacity, block)
        rows = rows.astype(jnp.bfloat16)
        total = jnp.dot(mix_high[...], rows, preferred_element_type=jnp.float32)
        total = total + jnp.dot(mix_low[...], rows, preferred_element_type=jnp.float32)
        mixed[:, cols] = total.astype(jnp.bfloat16)
        return carry

    lax.fori_loop(0, width // block, mix, 0)

    def drain(step, carry):
        to = peer(step)
        slot_copy(to, me).wait_send()
        first_copy(to, mine).wait_send()
        second_copy(to, mine).wait_send()
        back_copy(to, me).wait_send()
        return carry

    lax.fori_loop(1, n, drain, 0)
    for store in stores:
        store.wait()


def direct_shards(
    tokens, routes, route_weight, norm_gain, gate_weight, up_weight, down_weight
):
    n_fs, n_tp = lax.axis_size("fs"), lax.axis_size("tp")
    n = n_fs * n_tp
    tok_rows, width = tokens.shape
    tile_rows, tile_cols = gate_weight.shape[1:]
    down_rows, down_cols = down_weight.shape[1:]
    hidden = n_tp * tile_cols
    capacity = max(2, 3 * tok_rows * routes.shape[1] // (2 * n))
    bf16, f32 = jnp.bfloat16, jnp.float32
    whole = pl.BlockSpec(memory_space=pltpu.VMEM)
    apart = pl.BlockSpec(memory_space=pl.ANY)
    per_device = pltpu.SemaphoreType.DMA((n,))
    return pl.pallas_call(
        functools.partial(exchange_kernel, (n_fs, n_tp, capacity)),
        out_shape=(
            jax.ShapeDtypeStruct((1, width, hidden), bf16),
            jax.ShapeDtypeStruct((1, width, hidden), bf16),
            jax.ShapeDtypeStruct((1, hidden, width), bf16),
            jax.ShapeDtypeStruct((tok_rows, width), bf16),
        ),
        in_specs=[whole] * 4 + [apart] * 3,
        out_specs=(apart, apart, apart, whole),
        scratch_shapes=[
            pltpu.VMEM((n, tile_rows, tile_cols), f32),
            pltpu.VMEM((n, tile_rows, tile_cols), f32),
            pltpu.VMEM((n, down_rows, down_cols), f32),
            pltpu.VMEM((n, 2, tile_rows, tile_cols), bf16),
            pltpu.VMEM((n, down_rows, down_cols), bf16),
            pltpu.VMEM((2, width, hidden), bf16),
            pltpu.VMEM((hidden, width), bf16),
            pltpu.VMEM((n, capacity, width), bf16),
            pltpu.VMEM((n, capacity, width), bf16),
            pltpu.VMEM((n // 8, 8 * capacity, hidden), bf16),
            pltpu.VMEM((n, tok_rows), f32),
            pltpu.VMEM((n * capacity, tok_rows), f32),
            pltpu.VMEM((tok_rows, n * capacity), bf16),
            pltpu.VMEM((tok_rows, n * capacity), bf16),
            pltpu.VMEM((n, capacity, width), bf16),
            pltpu.VMEM((n, capacity, width), bf16),
            pltpu.SemaphoreType.DMA((3,)),
            pltpu.SemaphoreType.DMA((3,)),
        ]
        + [per_device] * 8,
        compiler_params=pltpu.CompilerParams(
            collective_id=0, has_side_effects=True, vmem_limit_bytes=60 * 1024 * 1024
        ),
    )(
        tokens,
        routes.T,
        route_weight.T,
        norm_gain[:, None],
        gate_weight,
        up_weight,
        down_weight,
    )


def aligned(mesh, tokens, routes, gate_weight, down_weight):
    n_fs, n_tp = mesh.shape["fs"], mesh.shape["tp"]
    n = n_fs * n_tp
    tok_rows = tokens.shape[0] // n
    capacity = max(2, 3 * tok_rows * routes.shape[1] // (2 * n))
    return (
        gate_weight.shape[0] == n
        and n % 8 == 0
        and capacity % 8 == 0
        and tok_rows % 128 == 0
        and tokens.shape[1] % 512 == 0
        and gate_weight.shape[1] // n_fs % 16 == 0
        and gate_weight.shape[2] // n_tp % 128 == 0
        and down_weight.shape[1] // n_fs % 16 == 0
        and down_weight.shape[2] // n_tp % 128 == 0
    )


def solution(mesh):
    placed = (
        P(("fs", "tp"), None),
        P(("fs", "tp"), None),
        P(("fs", "tp"), None),
        P("fs"),
        P(None, "fs", "tp"),
        P(None, "fs", "tp"),
        P(None, "fs", "tp"),
    )

    def run(tokens, routes, route_weight, norm_gain, gate_weight, up_weight, down_weight):
        direct = aligned(mesh, tokens, routes, gate_weight, down_weight)
        return jax.shard_map(
            direct_shards if direct else shards,
            mesh=mesh,
            in_specs=placed,
            out_specs=(
                P(("fs", "tp"), None, None),
                P(("fs", "tp"), None, None),
                P(("fs", "tp"), None, None),
                P(("fs", "tp"), None),
            ),
            check_vma=False,
        )(tokens, routes, route_weight, norm_gain, gate_weight, up_weight, down_weight)

    return run
```

```python
import functools

import jax
import jax.numpy as jnp
from jax import lax
from jax.experimental import pallas as pl
from jax.experimental.pallas import tpu as pltpu
from jax.sharding import PartitionSpec as P

norm_epsilon = 1e-06
clamp_limit = 7.0
sigmoid_slope = 1.702
MESH = pl.DeviceIdType.MESH


def feed(inputs, gate_mat, up_mat, down_mat):
    gate_pre = jnp.dot(inputs, gate_mat, preferred_element_type=jnp.float32)
    up_pre = jnp.dot(inputs, up_mat, preferred_element_type=jnp.float32)
    gate_part = jnp.minimum(gate_pre, clamp_limit)
    linear_part = jnp.clip(up_pre, -clamp_limit, clamp_limit)
    activation = (
        gate_part * jax.nn.sigmoid(sigmoid_slope * gate_part) * (linear_part + 1.0)
    ).astype(jnp.bfloat16)
    return jnp.dot(activation, down_mat, preferred_element_type=jnp.float32).astype(jnp.bfloat16)


def assemble(received, rows_groups, column_groups):
    tile_rows = received.shape[2]
    tile_columns = received.shape[3]
    sources = received.reshape(rows_groups, column_groups, tile_rows, tile_columns)
    return sources.transpose(0, 2, 1, 3).reshape(
        1, rows_groups * tile_rows, column_groups * tile_columns
    )


def shards(tokens, routes, route_weight, norm_gain, gate_weight, up_weight, down_weight):
    gain_column = norm_gain[None, :, None]
    gate_tiles = (gate_weight * gain_column).astype(jnp.bfloat16)
    up_tiles = (up_weight * gain_column).astype(jnp.bfloat16)
    down_tiles = down_weight.astype(jnp.bfloat16)
    rows_groups = lax.axis_size("fs")
    column_groups = lax.axis_size("tp")
    arrived = (
        lax.all_to_all(gate_tiles[:, None], ("fs", "tp"), split_axis=0, concat_axis=1, tiled=True),
        lax.all_to_all(up_tiles[:, None], ("fs", "tp"), split_axis=0, concat_axis=1, tiled=True),
        lax.all_to_all(down_tiles[:, None], ("fs", "tp"), split_axis=0, concat_axis=1, tiled=True),
    )
    gate_new = assemble(arrived[0], rows_groups, column_groups)
    up_new = assemble(arrived[1], rows_groups, column_groups)
    down_new = assemble(arrived[2], rows_groups, column_groups)
    experts = rows_groups * column_groups
    tok_rows, model_width = tokens.shape
    per_token = routes.shape[1]
    capacity = max(2, 3 * tok_rows * per_token // (2 * experts))
    values = tokens.astype(jnp.float32)
    squares = jnp.mean(values * values, axis=1, keepdims=True)
    normed = (values * lax.rsqrt(squares + norm_epsilon)).astype(jnp.bfloat16)
    flat_routes = routes.reshape(-1)
    onehot = (flat_routes[:, None] == jnp.arange(experts, dtype=jnp.int32)[None, :]).astype(
        jnp.int32
    )
    earlier = jnp.cumsum(onehot, axis=0) - onehot
    rank = jnp.sum(earlier * onehot, axis=1)
    slot_index = flat_routes * capacity + rank
    slot_numbers = jnp.arange(experts * capacity, dtype=jnp.int32)
    select = jnp.any(
        slot_index.reshape(tok_rows, per_token)[None, :, :] == slot_numbers[:, None, None], axis=2
    )
    buffer = jnp.dot(
        select.astype(jnp.bfloat16), normed, preferred_element_type=jnp.float32
    ).astype(jnp.bfloat16)
    buffer = buffer.reshape(experts, 1, capacity, model_width)
    slot_rows = lax.all_to_all(buffer, ("fs", "tp"), split_axis=0, concat_axis=1, tiled=True)
    sources = slot_rows.shape[1]
    count = slot_rows.shape[2]
    expert_out = feed(slot_rows.reshape(-1, model_width), gate_new[0], up_new[0], down_new[0])
    expert_out = expert_out.reshape(1, sources, count, model_width)
    returned = lax.all_to_all(expert_out, ("fs", "tp"), split_axis=1, concat_axis=0, tiled=True)
    returned = returned.reshape(experts * capacity, model_width)
    picked = returned[slot_index].reshape(tok_rows, per_token, model_width)
    mixed = jnp.sum(picked.astype(jnp.float32) * route_weight[:, :, None], axis=1).astype(
        jnp.bfloat16
    )
    return (gate_new, up_new, down_new, mixed)


def exchange_kernel(
    sizes, tokens, routes_t, weight_t, gain, gate, up, down,
    gate_out, up_out, down_out, mixed,
    gate_in, up_in, down_in, in_tiles, out_tiles, in_mats, out_mat,
    slots_out, slots_in, active, ranks, picks, mix_high, mix_low, rows_out, rows_in,
    normed_out, normed_in, far_routes, far_weight, part_out, part_in,
    trade_send, trade_recv, part_send, part_recv, load_sem, store_sem, slot_send, slot_recv, first_send, first_recv,
    second_send, second_recv, back_send, back_recv,
):
    n_fs, n_tp, capacity = sizes
    n = n_fs * n_tp
    fs, tp = lax.axis_index("fs"), lax.axis_index("tp")
    me = fs * n_tp + tp
    tok_rows, width = tokens.shape
    tile_rows, tile_cols = gate_in.shape[1:]
    down_rows, down_cols = down_in.shape[1:]
    group = 8
    groups = n // group
    group_rows = group * capacity

    half_fs, half_n = n_fs // 2, n // 2
    half, place = fs // half_fs, lax.rem(fs, half_fs)
    spot = place * n_tp + tp
    half_groups = half_n // group
    far = (lax.rem(fs + half_fs, n_fs), tp, lax.rem(me + half_n, n))

    def peer(step):
        local = lax.rem(step + step // half_n, half_n)
        side = lax.rem(half + 1 + step // half_n, 2)
        to_fs = side * half_fs + lax.rem(place + local // n_tp, half_fs)
        to_tp = lax.rem(tp + lax.rem(local, n_tp), n_tp)
        return to_fs, to_tp, to_fs * n_tp + to_tp

    barrier = pltpu.get_barrier_semaphore()

    def greet(step, carry):
        to_fs, to_tp, _ = peer(step)
        pl.semaphore_signal(barrier, inc=1, device_id=(to_fs, to_tp), device_id_type=MESH)
        return carry

    loads = [
        pltpu.make_async_copy(gate, gate_in, load_sem.at[0]),
        pltpu.make_async_copy(up, up_in, load_sem.at[1]),
        pltpu.make_async_copy(down, down_in, load_sem.at[2]),
    ]
    for load in loads:
        load.start()
    lax.fori_loop(0, n - 1, greet, 0)

    before = (
        lax.broadcasted_iota(jnp.int32, (tok_rows, tok_rows), 0)
        < lax.broadcasted_iota(jnp.int32, (tok_rows, tok_rows), 1)
    ).astype(jnp.float32).astype(jnp.bfloat16)
    experts = lax.broadcasted_iota(jnp.int32, (half_n, tok_rows), 0) + half * half_n

    def fill_slots(q, paths, shares, rows_ref):
        named = jnp.zeros((half_n, tok_rows), jnp.float32)
        scaled = jnp.zeros((half_n, tok_rows), jnp.float32)
        for k in range(paths.shape[0]):
            hit = paths[k : k + 1, :] == experts
            named = named + hit.astype(jnp.float32)
            scaled = scaled + jnp.where(hit, shares[k : k + 1, :], 0.0)
        rank = jnp.dot(named.astype(jnp.bfloat16), before, preferred_element_type=jnp.float32)
        ranks[q * half_n : (q + 1) * half_n, :] = jnp.where(named > 0.5, rank, -1.0)
        number = lax.broadcasted_iota(jnp.int32, (group, capacity, tok_rows), 1).astype(jnp.float32)
        for g in range(half_groups):
            held = slice(q * half_n + g * group, q * half_n + (g + 1) * group)
            select = (ranks[held, :][:, None, :] == number).astype(jnp.float32)
            start = (q * half_groups + g) * group_rows
            picks[start : start + group_rows, :] = (
                select * scaled[g * group : (g + 1) * group, :][:, None, :]
            ).reshape(group_rows, tok_rows)
            rows = jnp.dot(
                select.reshape(group_rows, tok_rows).astype(jnp.bfloat16),
                rows_ref[...],
                preferred_element_type=jnp.float32,
            )
            slots_out[held] = rows.reshape(group, capacity, width).astype(jnp.bfloat16)

    values = tokens[...].astype(jnp.float32)
    squares = jnp.mean(values * values, axis=1, keepdims=True)
    normed_out[...] = (values * lax.rsqrt(squares + norm_epsilon)).astype(jnp.bfloat16)

    def trade(number, source, target):
        return pltpu.make_async_remote_copy(
            src_ref=source,
            dst_ref=target,
            send_sem=trade_send.at[number],
            recv_sem=trade_recv.at[number],
            device_id=(far[0], far[1]),
            device_id_type=MESH,
        )

    trades = [
        trade(0, routes_t, far_routes),
        trade(1, weight_t, far_weight),
        trade(2, normed_out, normed_in),
    ]
    pl.semaphore_wait(barrier, n - 1)
    for each in trades:
        each.start()
    fill_slots(0, routes_t, weight_t, normed_out)

    def near(step):
        to_place = lax.rem(place + step // n_tp, half_fs)
        to_tp = lax.rem(tp + lax.rem(step, n_tp), n_tp)
        return half * half_fs + to_place, to_tp, to_place * n_tp + to_tp

    def slot_copy(q, to, source):
        block = q * half_n + to[2]
        return pltpu.make_async_remote_copy(
            src_ref=slots_out.at[block],
            dst_ref=slots_in.at[source],
            send_sem=slot_send.at[block],
            recv_sem=slot_recv.at[source],
            device_id=(to[0], to[1]),
            device_id_type=MESH,
        )

    def owner(q, at):
        return lax.rem(half + q, 2) * half_n + at

    def first_copy(to, place):
        return pltpu.make_async_remote_copy(
            src_ref=in_tiles.at[to[2]],
            dst_ref=in_mats.at[
                :,
                pl.ds(pl.multiple_of(place[0] * tile_rows, tile_rows), tile_rows),
                pl.ds(pl.multiple_of(place[1] * tile_cols, tile_cols), tile_cols),
            ],
            send_sem=first_send.at[to[2]],
            recv_sem=first_recv.at[place[2]],
            device_id=(to[0], to[1]),
            device_id_type=MESH,
        )

    def second_copy(to, place):
        return pltpu.make_async_remote_copy(
            src_ref=out_tiles.at[to[2]],
            dst_ref=out_mat.at[
                pl.ds(pl.multiple_of(place[0] * down_rows, down_rows), down_rows),
                pl.ds(pl.multiple_of(place[1] * down_cols, down_cols), down_cols),
            ],
            send_sem=second_send.at[to[2]],
            recv_sem=second_recv.at[place[2]],
            device_id=(to[0], to[1]),
            device_id_type=MESH,
        )

    def back_copy(source, block):
        to_spot = lax.rem(source, half_n)
        return pltpu.make_async_remote_copy(
            src_ref=rows_out.at[source],
            dst_ref=rows_in.at[block],
            send_sem=back_send.at[source],
            recv_sem=back_recv.at[block],
            device_id=(half * half_fs + to_spot // n_tp, lax.rem(to_spot, n_tp)),
            device_id_type=MESH,
        )

    mine = (fs, tp, me)

    def send_slots(q):
        def send_one(step, carry):
            slot_copy(q, near(step), owner(q, spot)).start()
            return carry

        lax.fori_loop(1, half_n, send_one, 0)
        slots_in[owner(q, spot)] = slots_out[q * half_n + spot]

    loads[0].wait()
    loads[1].wait()
    gains = jnp.broadcast_to(gain[...], (tile_rows, tile_cols))

    def cast_first(step):
        e = peer(step)[2]
        in_tiles[e, 0] = (gate_in[e] * gains).astype(jnp.bfloat16)
        in_tiles[e, 1] = (up_in[e] * gains).astype(jnp.bfloat16)

    cast_first(0)

    def send_first(step, carry):
        cast_first(step + 1)
        first_copy(peer(step), mine).start()
        return carry

    lax.fori_loop(0, half_n, send_first, 0)
    send_slots(0)
    for each in trades:
        each.wait_recv()
    fill_slots(1, far_routes, far_weight, normed_in)
    lax.fori_loop(half_n, n - 1, send_first, 0)
    send_slots(1)
    own_rows = pl.ds(pl.multiple_of(fs * tile_rows, tile_rows), tile_rows)
    own_cols = pl.ds(pl.multiple_of(tp * tile_cols, tile_cols), tile_cols)
    in_mats[0, own_rows, own_cols] = in_tiles[me, 0]
    in_mats[1, own_rows, own_cols] = in_tiles[me, 1]

    loads[2].wait()

    def cast_second(step):
        e = peer(step)[2]
        out_tiles[e] = down_in[e].astype(jnp.bfloat16)

    cast_second(0)

    def send_second(step, carry):
        cast_second(step + 1)
        second_copy(peer(step), mine).start()
        return carry

    lax.fori_loop(0, n - 1, send_second, 0)
    out_mat[
        pl.ds(pl.multiple_of(fs * down_rows, down_rows), down_rows),
        pl.ds(pl.multiple_of(tp * down_cols, down_cols), down_cols),
    ] = out_tiles[me]

    shares = jnp.transpose(picks[...])
    high = shares.astype(jnp.bfloat16)
    mix_high[...] = high
    mix_low[...] = (shares - high.astype(jnp.float32)).astype(jnp.bfloat16)

    def take_slots(step, carry):
        from_spot = near(step)[2]
        for q in range(2):
            slot_copy(q, near(step), owner(q, from_spot)).wait_recv()
        return carry

    lax.fori_loop(1, half_n, take_slots, 0)

    def take_first(step, carry):
        first_copy(mine, peer(step)).wait_recv()
        return carry

    lax.fori_loop(0, n - 1, take_first, 0)
    stores = [
        pltpu.make_async_copy(in_mats.at[0], gate_out.at[0], store_sem.at[0]),
        pltpu.make_async_copy(in_mats.at[1], up_out.at[0], store_sem.at[1]),
        pltpu.make_async_copy(out_mat, down_out.at[0], store_sem.at[2]),
    ]
    stores[0].start()
    stores[1].start()

    def activate(g, carry):
        inputs = slots_in[pl.ds(g * group, group)].astype(jnp.float32)
        inputs = inputs.reshape(group_rows, width).astype(jnp.bfloat16)
        gate_pre = jnp.dot(inputs, in_mats[0], preferred_element_type=jnp.float32)
        up_pre = jnp.dot(inputs, in_mats[1], preferred_element_type=jnp.float32)
        gate_part = jnp.minimum(gate_pre, clamp_limit)
        linear_part = jnp.clip(up_pre, -clamp_limit, clamp_limit)
        active[g] = (
            gate_part * jax.nn.sigmoid(sigmoid_slope * gate_part) * (linear_part + 1.0)
        ).astype(jnp.bfloat16)
        return carry

    lax.fori_loop(0, groups, activate, 0)

    def take_second(step, carry):
        second_copy(mine, peer(step)).wait_recv()
        return carry

    lax.fori_loop(0, n - 1, take_second, 0)
    stores[2].start()
    home = (1 - half) * half_groups

    def project(c):
        g = lax.rem(home + c, groups)
        rows = jnp.dot(active[g], out_mat[...], preferred_element_type=jnp.float32)
        rows_out[pl.ds(g * group, group)] = rows.reshape(group, capacity, width).astype(
            jnp.bfloat16
        )

    def send_group(c):
        g = lax.rem(home + c, groups)

        def send_back(step, carry):
            source = g * group + lax.rem(me + step, group)
            crossing = lax.rem(source // half_n + half, 2)

            @pl.when(lax.rem(source, half_n) != spot)
            def _():
                back_copy(source, crossing * half_n + spot).start()

            return carry

        lax.fori_loop(0, group, send_back, 0)

    project(0)

    def return_group(c, carry):
        project(c)
        send_group(c - 1)
        return carry

    lax.fori_loop(1, groups, return_group, 0)
    send_group(groups - 1)
    for q in range(2):
        rows_in[q * half_n + spot] = rows_out[owner(q, spot)]
    block = 512
    span = half_n * capacity

    def combine(q, cols):
        rows = rows_in[q * half_n : (q + 1) * half_n, :, cols].astype(jnp.float32)
        rows = rows.reshape(span, block).astype(jnp.bfloat16)
        taken = slice(q * span, (q + 1) * span)
        total = jnp.dot(mix_high[:, taken], rows, preferred_element_type=jnp.float32)
        return total + jnp.dot(mix_low[:, taken], rows, preferred_element_type=jnp.float32)

    def take_back(q):
        def take_one(step, carry):
            back_copy(owner(q, spot), q * half_n + near(step)[2]).wait_recv()
            return carry

        lax.fori_loop(1, half_n, take_one, 0)

    def part_copy(c):
        cols = slice(c * block, (c + 1) * block)
        return pltpu.make_async_remote_copy(
            src_ref=part_out.at[:, cols],
            dst_ref=part_in.at[:, cols],
            send_sem=part_send.at[c],
            recv_sem=part_recv.at[c],
            device_id=(far[0], far[1]),
            device_id_type=MESH,
        )

    take_back(1)
    for c in range(width // block):
        cols = slice(c * block, (c + 1) * block)
        part_out[:, cols] = combine(1, cols).astype(jnp.bfloat16)
        if c > 0:
            part_copy(c - 1).start()
    part_copy(width // block - 1).start()
    take_back(0)
    for c in range(width // block):
        cols = slice(c * block, (c + 1) * block)
        total = combine(0, cols)
        part_copy(c).wait_recv()
        mixed[:, cols] = (total + part_in[:, cols].astype(jnp.float32)).astype(jnp.bfloat16)

    def drain(step, carry):
        to = peer(step)
        first_copy(to, mine).wait_send()
        second_copy(to, mine).wait_send()
        return carry

    lax.fori_loop(0, n - 1, drain, 0)

    def drain_near(step, carry):
        to = near(step)
        for q in range(2):
            slot_copy(q, to, owner(q, spot)).wait_send()
            back_copy(owner(q, to[2]), q * half_n + spot).wait_send()
        return carry

    lax.fori_loop(1, half_n, drain_near, 0)
    for each in trades:
        each.wait_send()
    for c in range(width // block):
        part_copy(c).wait_send()
    for store in stores:
        store.wait()


def direct_shards(
    tokens, routes, route_weight, norm_gain, gate_weight, up_weight, down_weight
):
    n_fs, n_tp = lax.axis_size("fs"), lax.axis_size("tp")
    n = n_fs * n_tp
    tok_rows, width = tokens.shape
    tile_rows, tile_cols = gate_weight.shape[1:]
    down_rows, down_cols = down_weight.shape[1:]
    hidden = n_tp * tile_cols
    capacity = max(2, 3 * tok_rows * routes.shape[1] // (2 * n))
    bf16, f32 = jnp.bfloat16, jnp.float32
    whole = pl.BlockSpec(memory_space=pltpu.VMEM)
    apart = pl.BlockSpec(memory_space=pl.ANY)
    per_device = pltpu.SemaphoreType.DMA((n,))
    return pl.pallas_call(
        functools.partial(exchange_kernel, (n_fs, n_tp, capacity)),
        out_shape=(
            jax.ShapeDtypeStruct((1, width, hidden), bf16),
            jax.ShapeDtypeStruct((1, width, hidden), bf16),
            jax.ShapeDtypeStruct((1, hidden, width), bf16),
            jax.ShapeDtypeStruct((tok_rows, width), bf16),
        ),
        in_specs=[whole] * 4 + [apart] * 3,
        out_specs=(apart, apart, apart, whole),
        scratch_shapes=[
            pltpu.VMEM((n, tile_rows, tile_cols), f32),
            pltpu.VMEM((n, tile_rows, tile_cols), f32),
            pltpu.VMEM((n, down_rows, down_cols), f32),
            pltpu.VMEM((n, 2, tile_rows, tile_cols), bf16),
            pltpu.VMEM((n, down_rows, down_cols), bf16),
            pltpu.VMEM((2, width, hidden), bf16),
            pltpu.VMEM((hidden, width), bf16),
            pltpu.VMEM((n, capacity, width), bf16),
            pltpu.VMEM((n, capacity, width), bf16),
            pltpu.VMEM((n // 8, 8 * capacity, hidden), bf16),
            pltpu.VMEM((n, tok_rows), f32),
            pltpu.VMEM((n * capacity, tok_rows), f32),
            pltpu.VMEM((tok_rows, n * capacity), bf16),
            pltpu.VMEM((tok_rows, n * capacity), bf16),
            pltpu.VMEM((n, capacity, width), bf16),
            pltpu.VMEM((n, capacity, width), bf16),
            pltpu.VMEM((tok_rows, width), bf16),
            pltpu.VMEM((tok_rows, width), bf16),
            pltpu.VMEM((routes.shape[1], tok_rows), routes.dtype),
            pltpu.VMEM((routes.shape[1], tok_rows), f32),
            pltpu.VMEM((tok_rows, width), bf16),
            pltpu.VMEM((tok_rows, width), bf16),
            pltpu.SemaphoreType.DMA((3,)),
            pltpu.SemaphoreType.DMA((3,)),
            pltpu.SemaphoreType.DMA((width // 512,)),
            pltpu.SemaphoreType.DMA((width // 512,)),
            pltpu.SemaphoreType.DMA((3,)),
            pltpu.SemaphoreType.DMA((3,)),
        ]
        + [per_device] * 8,
        compiler_params=pltpu.CompilerParams(
            collective_id=0, has_side_effects=True, vmem_limit_bytes=60 * 1024 * 1024
        ),
    )(
        tokens,
        routes.T,
        route_weight.T,
        norm_gain[:, None],
        gate_weight,
        up_weight,
        down_weight,
    )


def aligned(mesh, tokens, routes, gate_weight, down_weight):
    n_fs, n_tp = mesh.shape["fs"], mesh.shape["tp"]
    n = n_fs * n_tp
    tok_rows = tokens.shape[0] // n
    capacity = max(2, 3 * tok_rows * routes.shape[1] // (2 * n))
    return (
        gate_weight.shape[0] == n
        and n_fs % 2 == 0
        and n % 16 == 0
        and capacity % 8 == 0
        and tok_rows % 128 == 0
        and tokens.shape[1] % 512 == 0
        and gate_weight.shape[1] // n_fs % 16 == 0
        and gate_weight.shape[2] // n_tp % 128 == 0
        and down_weight.shape[1] // n_fs % 16 == 0
        and down_weight.shape[2] // n_tp % 128 == 0
    )


def solution(mesh):
    placed = (
        P(("fs", "tp"), None),
        P(("fs", "tp"), None),
        P(("fs", "tp"), None),
        P("fs"),
        P(None, "fs", "tp"),
        P(None, "fs", "tp"),
        P(None, "fs", "tp"),
    )

    def run(tokens, routes, route_weight, norm_gain, gate_weight, up_weight, down_weight):
        direct = aligned(mesh, tokens, routes, gate_weight, down_weight)
        return jax.shard_map(
            direct_shards if direct else shards,
            mesh=mesh,
            in_specs=placed,
            out_specs=(
                P(("fs", "tp"), None, None),
                P(("fs", "tp"), None, None),
                P(("fs", "tp"), None, None),
                P(("fs", "tp"), None),
            ),
            check_vma=False,
        )(tokens, routes, route_weight, norm_gain, gate_weight, up_weight, down_weight)

    return run
```
